32 devices in a mesh: sp: 8 (over z, x), tp: 4 (over y, core).
Axes of the slice: x: 2, y: 2, z: 4, core: 2. Of those that a mesh axis runs over, the one named last changes fastest.
Arguments:
- resid: bfloat16 [1024, 2048], P('sp'), may hold values from -6 to 6
- norm_gain: float32 [2048], replicated, may hold values from 0.1 to 1.9
- cotangent: bfloat16 [1024, 2048], P('sp'), may hold values from -6 to 6
- route_ids: int32 [1024, 2], P('sp'), may hold values from 0 to 7, all different within a row; in each aligned block of 128 rows (0 to 127, 128 to 255, ...) at most 48 rows name the same one
- route_weight: float32 [1024, 2], P('sp'), may hold values from 0.25 to 2.25
- expert_gate: bfloat16 [8, 2048, 2048], P('sp', None, 'tp'), may hold values from -0.125 to 0.125
- expert_up: bfloat16 [8, 2048, 2048], P('sp', None, 'tp'), may hold values from -0.125 to 0.125
- expert_down: bfloat16 [8, 2048, 2048], P('sp', 'tp'), may hold values from -0.125 to 0.125
- out_proj: bfloat16 [2048, 4096], P('sp', 'tp'), may hold values from -0.09375 to 0.09375
- mixed: bfloat16 [1024, 4096], P('sp', 'tp'), may hold values from -6 to 6
- query: bfloat16 [1024, 2048], P('sp', 'tp'), may hold values from -6 to 6
- key: bfloat16 [1024, 2048], P('sp', 'tp'), may hold values from -1.5 to 1.5
- value: bfloat16 [1024, 4096], P('sp', 'tp'), may hold values from -6 to 6
- log_decay: float32 [1024, 2048], P('sp', 'tp'), may hold values from -1 to 0, as said below
- span_state: float32 [8, 16, 128, 256], P('sp', 'tp'), may hold values from -24 to 24
Outputs:
- grad_expert_gate: bfloat16 [8, 2048, 2048], P('sp', None, 'tp')
- grad_expert_up: bfloat16 [8, 2048, 2048], P('sp', None, 'tp')
- grad_expert_down: bfloat16 [8, 2048, 2048], P('sp', 'tp')
- grad_out_proj: float32 [2048, 4096], P('sp', 'tp')
- grad_query: bfloat16 [1024, 2048], P('sp', 'tp')
- grad_key: bfloat16 [1024, 2048], P('sp', 'tp')
- grad_value: bfloat16 [1024, 4096], P('sp', 'tp')
- grad_log_decay: float32 [1024, 2048], P('sp', 'tp')
The draws below stay inside these ranges and needn't reach their ends.
Inputs may be any that keep to these rules, and one draw needn't show every extreme that they name: `route_ids`: A row names 2 different experts. Within each aligned block of 128 rows (the rows of one index of sp) no expert is named by more than 48 rows, and in every draw some expert is named by exactly 48 rows of some block. `log_decay`: every entry is zero or negative.
All inputs are finite; a program needn't handle non-finite values.
Results may differ from the reference program's by a relative error of at most 0.023.
Values may be sent and summed in bfloat16 or wider, within the bound.
A program may use at most 128 MiB of HBM per device.

```python
import math
import jax
import jax.numpy as jnp
import numpy as np
from jax import lax

D = 2048
ATTENTION_HEADS = 16
KEY_CHANNELS = 128
DV = 256
FE = 2048
TOP = 2
BLOCK = 64
TOK_DEV = 128
EXPERTS = 8
TOKEN_POSITIONS = 1024
CAP = 48
SPANS = 8
N_SP = 8
N_TP = 4


def draw_log_decay(key, part):
    random_keys = jax.random.split(jax.random.fold_in(key, 17), 8)
    fast_share = 0.5
    slow_base = jnp.exp(jax.random.uniform(random_keys[1], (ATTENTION_HEADS, KEY_CHANNELS), jnp.float32, jnp.log(0.1), jnp.log(0.6))) / TOKEN_POSITIONS
    fast_base = jnp.exp(jax.random.uniform(random_keys[2], (ATTENTION_HEADS, KEY_CHANNELS), jnp.float32, jnp.log(1.0 / 80.0), jnp.log(1.0 / 40.0)))
    fast_heads = jax.random.bernoulli(random_keys[0], fast_share, (ATTENTION_HEADS,))
    base_rate = jnp.where(fast_heads[:, None], fast_base, slow_base)
    span_factor = jnp.exp(jax.random.uniform(random_keys[3], (TOKEN_POSITIONS // TOK_DEV, 1, 1), jnp.float32, jnp.log(0.5), jnp.log(2.0)))
    span_factor = jnp.repeat(span_factor, TOK_DEV, axis=0)
    position_factor = jax.random.uniform(random_keys[4], (TOKEN_POSITIONS, ATTENTION_HEADS, KEY_CHANNELS), jnp.float32, 0.5, 1.5)
    decay_speeds = base_rate[None, :, :] * span_factor * position_factor
    cluster_start = jax.random.randint(random_keys[5], (ATTENTION_HEADS, 1), 0, TOKEN_POSITIONS)
    cluster_spacing = jax.random.randint(random_keys[7], (ATTENTION_HEADS, 1), 1, TOKEN_POSITIONS)
    cluster_location = jnp.concatenate([cluster_start, (cluster_start + cluster_spacing) % TOKEN_POSITIONS], axis=1)
    cluster_length = jax.random.uniform(random_keys[6], (ATTENTION_HEADS, 2), jnp.float32, 0.22, 0.69)
    token_places = jnp.arange(TOKEN_POSITIONS, dtype=jnp.int32)[:, None, None]
    cluster_count = jnp.sum(jnp.where(token_places == cluster_location[None, :, :], cluster_length[None, :, :], 0.0), axis=2)
    return (-(decay_speeds + cluster_count[:, :, None])).reshape(TOKEN_POSITIONS, ATTENTION_HEADS * KEY_CHANNELS).astype(jnp.float32)


def spiked(entries, key, source, target, blocks, factor):
    def block_of(dim):
        return (jnp.arange(entries.shape[dim]) // (entries.shape[dim] // blocks)).reshape((-1,) + (1,) * (entries.ndim - 1 - dim))

    one_side = jax.random.permutation(key, blocks)[block_of(target)]
    other_side = (block_of(target) + blocks // 2) % blocks
    return jnp.where((block_of(source) == one_side) | (block_of(source) == other_side), factor * entries, entries)


def levels(key, dims, cuts, least, top_value):
    level = 1.0
    for dim, shards_of in cuts:
        heights = jax.random.uniform(jax.random.fold_in(jax.random.fold_in(key, 6), dim), (shards_of,), jnp.float32, least / len(cuts), top_value / len(cuts))
        level = level * jnp.repeat(jnp.exp(heights), dims[dim] // shards_of).reshape((-1,) + (1,) * (len(dims) - 1 - dim))
    return level


def shared_out(key, own, number, rows, count, top, limit, slope):
    order = jax.random.permutation(key, count)
    packed, ordinary = portions_of(count, rows * top, limit, slope, True), portions_of(count, rows * top, limit, slope, False)
    places = jnp.arange(count)

    def named(tallies, turn):
        used = int((tallies > 0).sum())
        fixed = max(1, used // 4)
        moved = fixed + (places - fixed + turn * (used - fixed)) % max(1, count - fixed)
        return jnp.zeros((count,), jnp.int32).at[order[jnp.where(places < fixed, places, moved)]].set(jnp.asarray(tallies, jnp.int32))

    tallies = jnp.where(number % 4 == 0, named(packed, number // 4), named(ordinary, number - number // 4 - 1))
    mixed = jax.random.permutation(jax.random.fold_in(own, 3), count)
    donor, receiver = mixed[0:count // 2 * 2:2], mixed[1:count // 2 * 2:2]
    margin = jnp.minimum(tallies[donor] - 1, limit - tallies[receiver]) // 2
    margin = jnp.where((donor == order[0]) | (receiver == order[0]) | (tallies[receiver] == 0), 0, jnp.maximum(margin, 0))
    moved = jax.random.randint(jax.random.fold_in(own, 4), (count // 2,), 0, 1 << 20) % (margin + 1)
    tallies = tallies.at[donor].add(-moved).at[receiver].add(moved)
    labels = jnp.searchsorted(jnp.cumsum(tallies), jnp.arange(rows * top), side="right").astype(jnp.int32)
    table = labels.reshape(top, rows).T
    table = table[jax.random.permutation(jax.random.fold_in(own, 1), rows)]
    turn = jax.random.randint(jax.random.fold_in(own, 2), (rows, 1), 0, top)
    return jnp.take_along_axis(table, (jnp.arange(top)[None, :] + turn) % top, axis=1)


def portions_of(count, total, reach, lean, full):
    weights = [(1 << 20) // math.isqrt(grade ** lean) + 1 for grade in range(1, count + 1)]
    largest = reach if full else min(reach, max(-(-total // count), total * weights[0] // sum(weights)))
    least = 1 if total - largest >= count - 1 else 0
    holding, surplus = [largest] + [least] * (count - 1), total - largest - least * (count - 1)
    while surplus > 0:
        candidates = [i for i in range(1, count) if holding[i] < largest] or [i for i in range(1, count) if holding[i] < reach]
        mass, budget = sum([weights[i] for i in candidates]), surplus
        for i in candidates:
            extra = min(reach - holding[i], max(1, budget * weights[i] // mass), surplus)
            holding[i] = holding[i] + extra
            surplus = surplus - extra
    return np.array(holding)


def scatter_about(rng, shape, scale, bound, pieces=(), kind=jnp.bfloat16):
    loudness = levels(rng, shape, pieces, -0.22, 0.18) if pieces else 1.0
    drawn = jax.random.normal(rng, shape, jnp.float32) * scale * loudness
    return jnp.minimum(jnp.maximum(drawn, -bound), bound).astype(kind)


def bell_draw_with(own_key, dims, spread, bound, pieces, heavy, kind=jnp.bfloat16):
    values = spread * jax.random.normal(own_key, dims, jnp.float32)
    if pieces:
        values = values * levels(own_key, dims, pieces, -0.22, 0.18)
    return jnp.clip(spiked(values, jax.random.fold_in(own_key, 3), *heavy), -bound, bound).astype(kind)


def setup_inputs(seed: int = 0) -> dict:
    streams_of = jax.random.split(jax.random.key(seed), 16)
    resid = scatter_about(streams_of[0], (TOKEN_POSITIONS, D), 1.0, 6.0, ((0, 8),))
    norm_gain = jnp.clip(1.0 + 0.18 * jax.random.normal(streams_of[1], (D,), jnp.float32), 0.1, 1.9)
    cotangent = bell_draw_with(streams_of[2], (TOKEN_POSITIONS, D), 1.0, 6.0, ((0, 8),), (0, 1, 8, 2.0))
    route_ids_keys = jax.random.split(jax.random.fold_in(streams_of[3], 1), TOKEN_POSITIONS // TOK_DEV)
    route_ids_turns = jax.random.permutation(jax.random.fold_in(streams_of[3], 3), TOKEN_POSITIONS // TOK_DEV)
    route_ids = jax.vmap(lambda own, number: shared_out(jax.random.fold_in(streams_of[3], 2), own, number, TOK_DEV, EXPERTS, TOP, CAP, 2))(route_ids_keys, route_ids_turns).reshape((TOKEN_POSITIONS, TOP))
    route_weight = jnp.clip(0.25 + 2.0 * jax.random.uniform(streams_of[4], (TOKEN_POSITIONS, TOP), jnp.float32) ** levels(streams_of[4], (TOKEN_POSITIONS, TOP), ((0, 8),), -0.2, 0.2), 0.25, 2.25)
    expert_gate = scatter_about(streams_of[5], (EXPERTS, D, FE), D ** -0.5, 0.125, ((0, 8), (2, 4)))
    expert_up = scatter_about(streams_of[6], (EXPERTS, D, FE), D ** -0.5, 0.125, ((0, 8), (2, 4)))
    expert_down = scatter_about(streams_of[7], (EXPERTS, FE, D), FE ** -0.5, 0.125, ((0, 8), (1, 4)))
    out_proj = scatter_about(streams_of[8], (D, ATTENTION_HEADS * DV), (ATTENTION_HEADS * DV) ** -0.5, 0.09375, ((0, 8), (1, 4)))
    mixed = scatter_about(streams_of[9], (TOKEN_POSITIONS, ATTENTION_HEADS * DV), 1.0, 6.0, ((0, 8), (1, 4)))
    query = scatter_about(streams_of[10], (TOKEN_POSITIONS, ATTENTION_HEADS * KEY_CHANNELS), 1.0, 6.0, ((0, 8), (1, 4)))
    key = scatter_about(streams_of[11], (TOKEN_POSITIONS, ATTENTION_HEADS * KEY_CHANNELS), 0.25, 1.5, ((0, 8), (1, 4)))
    value = scatter_about(streams_of[12], (TOKEN_POSITIONS, ATTENTION_HEADS * DV), 1.0, 6.0, ((0, 8), (1, 4)))
    log_decay = draw_log_decay(jax.random.fold_in(streams_of[15], 71), 0)
    span_state = scatter_about(streams_of[14], (SPANS, ATTENTION_HEADS, KEY_CHANNELS, DV), 4.0, 24.0, ((0, 8), (1, 4)), jnp.float32)
    return {"resid": resid, "norm_gain": norm_gain, "cotangent": cotangent, "route_ids": route_ids, "route_weight": route_weight, "expert_gate": expert_gate, "expert_up": expert_up, "expert_down": expert_down, "out_proj": out_proj, "mixed": mixed, "query": query, "key": key, "value": value, "log_decay": log_decay, "span_state": span_state}


epsilon = 1e-06
highest = lax.Precision.HIGHEST

def rounded(values):
    return lax.optimization_barrier(values.astype(jnp.bfloat16)).astype(jnp.float32)

def into_blocks(values):
    return values.reshape(values.shape[0] // BLOCK, BLOCK, values.shape[1])

def span_forward(query_rows, key_rows, value_rows, grad_rows, decay_rows, entry_state):
    query_blk = into_blocks(query_rows)
    key_blk = into_blocks(key_rows)
    value_blk = into_blocks(value_rows)
    grad_blk = into_blocks(grad_rows)
    cumlog = jnp.cumsum(into_blocks(decay_rows), axis=1)
    block_total = cumlog[:, -1, :]
    to_end = jnp.exp(block_total[:, None, :] - cumlog)
    inner_part = jnp.einsum('nsd,nsj->ndj', key_blk * to_end, value_blk, precision=highest)

    def forward_step(carry_state, step_item):
        piece_part, block_sum = step_item
        return (jnp.exp(block_sum)[:, None] * carry_state + piece_part, carry_state)
    end_state, starts = lax.scan(forward_step, entry_state, (inner_part, block_total))
    own_part = jnp.einsum('ntd,ntj->ndj', query_blk * jnp.exp(cumlog), grad_blk, precision=highest)

    def backward_step(carry_state, step_item):
        piece_part, block_sum = step_item
        return (jnp.exp(block_sum)[:, None] * carry_state + piece_part, carry_state)
    start_cot, after_cot = lax.scan(backward_step, jnp.zeros_like(entry_state), (own_part, block_total), reverse=True)
    span_total = lax.optimization_barrier(jnp.sum(block_total, axis=0))
    later_log = span_total[None, :] - jnp.cumsum(block_total, axis=0)
    return ((cumlog, starts, after_cot, later_log, end_state), (jnp.exp(span_total), start_cot))

def span_backward(query_rows, key_rows, value_rows, grad_rows, kept_terms, exit_cot):
    cumlog, starts, after_cot, later_log, end_state = kept_terms
    query_blk = into_blocks(query_rows)
    key_blk = into_blocks(key_rows)
    value_blk = into_blocks(value_rows)
    grad_blk = into_blocks(grad_rows)
    exit_cots = after_cot + jnp.exp(later_log)[:, :, None] * exit_cot
    causal = jnp.arange(BLOCK)[:, None] >= jnp.arange(BLOCK)[None, :]
    decays = jnp.exp(jnp.where(causal[None, :, :, None], cumlog[:, :, None, :] - cumlog[:, None, :, :], -jnp.inf))
    scores = jnp.einsum('ntd,nsd,ntsd->nts', query_blk, key_blk, decays, precision=highest)
    grad_scores = jnp.einsum('ntj,nsj->nts', grad_blk, value_blk, precision=highest)
    grad_query = jnp.exp(cumlog) * jnp.einsum('ntj,ndj->ntd', grad_blk, starts, precision=highest)
    grad_query = grad_query + jnp.einsum('nts,nsd,ntsd->ntd', grad_scores, key_blk, decays, precision=highest)
    to_end = jnp.exp(cumlog[:, -1:, :] - cumlog)
    grad_key = jnp.einsum('nts,ntd,ntsd->nsd', grad_scores, query_blk, decays, precision=highest)
    grad_key = grad_key + to_end * jnp.einsum('nsj,ndj->nsd', value_blk, exit_cots, precision=highest)
    grad_value = jnp.einsum('nts,ntj->nsj', scores, grad_blk, precision=highest)
    grad_value = grad_value + jnp.einsum('nsd,ndj->nsj', key_blk * to_end, exit_cots, precision=highest)
    length = query_rows.shape[0]
    key_width = query_rows.shape[1]
    per_position = (query_blk * grad_query - key_blk * grad_key).reshape(length, key_width)
    grad_log = jnp.flip(jnp.cumsum(jnp.flip(per_position, 0), 0), 0) + lax.optimization_barrier(jnp.sum(end_state * exit_cot, axis=1))[None, :]
    return (grad_query.reshape(length, key_width), grad_key.reshape(length, key_width), grad_value.reshape(length, value_rows.shape[1]), grad_log)

def reference(resid, norm_gain, cotangent, route_ids, route_weight, expert_gate, expert_up, expert_down, out_proj, mixed, query, key, value, log_decay, span_state):
    resid_f = resid.astype(jnp.float32)
    inverse_rms = lax.rsqrt(lax.optimization_barrier(jnp.mean(resid_f * resid_f, axis=1, keepdims=True)) + epsilon)
    unit_rows = resid_f * inverse_rms
    normed = (unit_rows * norm_gain.astype(jnp.float32)).astype(jnp.bfloat16)
    sent_cot = (route_weight[:, :, None] * cotangent.astype(jnp.float32)[:, None, :]).astype(jnp.bfloat16)
    pair_expert = route_ids.reshape(N_SP, TOK_DEV * TOP)
    onehot = (pair_expert[:, :, None] == jnp.arange(EXPERTS, dtype=jnp.int32)[None, None, :]).astype(jnp.int32)
    slot_rank = lax.optimization_barrier(jnp.sum((jnp.cumsum(onehot, axis=1) - onehot) * onehot, axis=2))
    source = jnp.arange(N_SP, dtype=jnp.int32)[:, None]
    slot_index = ((pair_expert * N_SP + source) * CAP + slot_rank).astype(jnp.int32)
    pair_index = jnp.arange(TOKEN_POSITIONS * TOP, dtype=jnp.int32).reshape(N_SP, TOK_DEV * TOP)
    slot_table = jnp.full((EXPERTS * N_SP * CAP,), TOKEN_POSITIONS * TOP, jnp.int32)
    slot_table = slot_table.at[slot_index.reshape(-1)].set(pair_index.reshape(-1)).reshape(EXPERTS, N_SP * CAP)
    pair_rows = jnp.concatenate([jnp.repeat(normed, TOP, axis=0), jnp.zeros((1, D), jnp.bfloat16)], axis=0)
    pair_cots = jnp.concatenate([sent_cot.reshape(TOKEN_POSITIONS * TOP, D), jnp.zeros((1, D), jnp.bfloat16)], axis=0)
    group_width = FE // N_TP

    def one_expert(step_item):
        gate_w, up_w, down_w, slots = step_item
        rows_in = pair_rows[slots].astype(jnp.float32)
        rows_cot = pair_cots[slots].astype(jnp.float32)
        gate_f = gate_w.astype(jnp.float32)
        up_f = up_w.astype(jnp.float32)
        gate_pre = jnp.dot(rows_in, gate_f)
        up_pre = jnp.dot(rows_in, up_f)
        gate_sig = jax.nn.sigmoid(gate_pre)
        hidden = rounded(gate_pre * gate_sig * up_pre)
        grad_hidden = jnp.dot(rows_cot, down_w.astype(jnp.float32).T)
        grad_up_act = rounded(grad_hidden * gate_pre * gate_sig)
        grad_gate_act = rounded(grad_hidden * up_pre * gate_sig * (1.0 + gate_pre * (1.0 - gate_sig)))
        grad_down = jnp.dot(hidden.T, rows_cot).astype(jnp.bfloat16)
        grad_gate = jnp.dot(rows_in.T, grad_gate_act).astype(jnp.bfloat16)
        grad_up = jnp.dot(rows_in.T, grad_up_act).astype(jnp.bfloat16)
        rows_count = rows_in.shape[0]
        partial_value = jnp.einsum('rgf,dgf->grd', grad_gate_act.reshape(rows_count, N_TP, group_width), gate_f.reshape(D, N_TP, group_width))
        partial_value = partial_value + jnp.einsum('rgf,dgf->grd', grad_up_act.reshape(rows_count, N_TP, group_width), up_f.reshape(D, N_TP, group_width))
        pair_grad = lax.optimization_barrier(jnp.sum(rounded(partial_value), axis=0)).astype(jnp.bfloat16)
        return (grad_gate, grad_up, grad_down, pair_grad)
    grad_gate_all, grad_up_all, grad_down_all, pair_grads = lax.map(one_expert, (expert_gate, expert_up, expert_down, slot_table))
    pair_total = jnp.zeros((TOKEN_POSITIONS * TOP + 1, D), jnp.float32)
    pair_total = pair_total.at[slot_table.reshape(-1)].add(pair_grads.reshape(-1, D).astype(jnp.float32))
    grad_normed = lax.optimization_barrier(jnp.sum(pair_total[:-1].reshape(TOKEN_POSITIONS, TOP, D), axis=1))
    scaled = grad_normed * norm_gain.astype(jnp.float32)
    grad_resid = cotangent.astype(jnp.float32) + inverse_rms * (scaled - unit_rows * lax.optimization_barrier(jnp.mean(scaled * unit_rows, axis=1, keepdims=True)))
    grad_resid = grad_resid.astype(jnp.bfloat16)
    grad_out_proj = jnp.dot(grad_resid.T, mixed, preferred_element_type=jnp.float32)
    grad_mixed = jnp.dot(grad_resid, out_proj, preferred_element_type=jnp.float32).astype(jnp.bfloat16)
    query_scale = KEY_CHANNELS ** (-0.5)

    def heads_first(values, head_depth):
        return values.reshape(N_SP, TOK_DEV, ATTENTION_HEADS, head_depth).transpose(2, 0, 1, 3)

    def head_grads(step_item):
        query_h, key_h, value_h, grad_h, decay_h, state_h = step_item

        def span_step(exit_cot, span_item):
            query_p, key_p, value_p, grad_p, decay_p, entry_state = span_item
            query_rows = query_p.astype(jnp.float32) * query_scale
            key_rows = key_p.astype(jnp.float32)
            value_rows = value_p.astype(jnp.float32)
            grad_rows = grad_p.astype(jnp.float32)
            kept_terms, summary = span_forward(query_rows, key_rows, value_rows, grad_rows, decay_p, entry_state)
            span_grads = span_backward(query_rows, key_rows, value_rows, grad_rows, kept_terms, exit_cot)
            return (summary[0][:, None] * exit_cot + summary[1], span_grads)
        carry_end, span_grads = lax.scan(span_step, jnp.zeros((KEY_CHANNELS, DV), jnp.float32), (query_h, key_h, value_h, grad_h, decay_h, state_h), reverse=True)
        return span_grads
    grads_query, grads_key, grads_value, grads_log = lax.map(head_grads, (heads_first(query, KEY_CHANNELS), heads_first(key, KEY_CHANNELS), heads_first(value, DV), heads_first(grad_mixed, DV), heads_first(log_decay, KEY_CHANNELS), span_state.transpose(1, 0, 2, 3)))

    def tokens_first(values):
        return values.transpose(1, 2, 0, 3).reshape(TOKEN_POSITIONS, -1)
    grad_query = (tokens_first(grads_query) * query_scale).astype(jnp.bfloat16)
    grad_key = tokens_first(grads_key).astype(jnp.bfloat16)
    grad_value = tokens_first(grads_value).astype(jnp.bfloat16)
    grad_log_decay = tokens_first(grads_log)
    return (grad_gate_all, grad_up_all, grad_down_all, grad_out_proj, grad_query, grad_key, grad_value, grad_log_decay)
```

```python
import jax
import jax.numpy as jnp
from jax import lax
from jax.experimental import pallas as pl
from jax.experimental.pallas import tpu as pltpu
from jax.sharding import PartitionSpec as P

KEY_CHANNELS = 128
DV = 256
TOP = 2


epsilon = 1e-06
highest = lax.Precision.HIGHEST


SIDE = 16


def triangle(length, upper):
    rows = lax.broadcasted_iota(jnp.int32, (length, length), 0)
    cols = lax.broadcasted_iota(jnp.int32, (length, length), 1)
    return rows <= cols if upper else rows >= cols


def dot(a, b, ca, cb, precision=None):
    return lax.dot_general(
        a, b, (((ca,), (cb,)), ((), ())), preferred_element_type=jnp.float32, precision=precision
    )


def short(values):
    return values.astype(jnp.bfloat16)


def summary_kernel(resid_ref, proj_ref, query_ref, decay_ref, grad_ref, cum_ref, out_ref):
    length = query_ref.shape[0]
    grad = short(dot(resid_ref[...], proj_ref[...], 1, 0))
    grad_ref[...] = grad
    ones = triangle(length, False).astype(jnp.float32)
    cum = dot(ones, decay_ref[...], 1, 0, highest)
    cum_ref[...] = cum
    query = query_ref[...].astype(jnp.float32) * KEY_CHANNELS ** (-0.5)
    out_ref[0, 0:KEY_CHANNELS, :] = short(dot(short(query * jnp.exp(cum)), grad, 0, 0))
    total = jnp.exp(cum[length - 1 : length, :])
    upper = short(total)
    lower = short(total - upper.astype(jnp.float32))
    both = jnp.concatenate([upper.astype(jnp.float32), lower.astype(jnp.float32)], axis=1)
    out_ref[0, KEY_CHANNELS : KEY_CHANNELS + SIDE, :] = short(
        jnp.broadcast_to(both, (SIDE, both.shape[1]))
    )


def gradient_kernel(
    me_ref, all_ref, grad_ref, query_ref, key_ref, value_ref, cum_ref, state_ref,
    out_query, out_key, out_value, out_log,
):
    count = all_ref.shape[0]
    length = query_ref.shape[0]
    me = me_ref[0]
    sides = all_ref[:, 0, KEY_CHANNELS : KEY_CHANNELS + SIDE, :].astype(jnp.float32)
    sides = sides[:, 0, :]
    factors = (sides[:, :KEY_CHANNELS] + sides[:, KEY_CHANNELS : 2 * KEY_CHANNELS]).T
    exit_cot = jnp.zeros((KEY_CHANNELS, DV), jnp.float32)
    for j in range(count - 1, 0, -1):
        later = factors[:, j : j + 1] * exit_cot + all_ref[j, 0, 0:KEY_CHANNELS, :].astype(
            jnp.float32
        )
        exit_cot = jnp.where(j > me, later, exit_cot)
    exit_short = short(exit_cot)
    query_scale = KEY_CHANNELS ** (-0.5)
    cum = cum_ref[...]
    last = cum[length - 1 : length, :]
    middle = cum[length // 2 - 1 : length // 2, :]
    query = query_ref[...].astype(jnp.float32) * query_scale
    key = key_ref[...].astype(jnp.float32)
    grad = grad_ref[...]
    value = value_ref[...]
    state = state_ref[0, 0]
    rise = jnp.exp(cum - middle)
    fall = jnp.exp(middle - cum)
    to_end = jnp.exp(last - cum)
    causal = triangle(length, False)
    query_part = short(query * rise)
    key_part = short(key * fall)
    scores = short(jnp.where(causal, dot(query_part, key_part, 1, 1), 0.0))
    grad_scores = short(jnp.where(causal, dot(grad, value, 1, 1), 0.0))
    grad_query = rise * dot(grad_scores, key_part, 1, 0)
    grad_query = grad_query + jnp.exp(cum) * dot(grad, short(state), 1, 1)
    from_exit = dot(value, exit_short, 1, 1)
    key_end = key * to_end
    grad_key = fall * dot(grad_scores, query_part, 0, 0) + to_end * from_exit
    grad_value = dot(scores, grad, 0, 0) + dot(short(key_end), exit_short, 1, 0)
    product = dot(jnp.ones((8, DV), jnp.float32), state * exit_cot, 1, 1, highest)[0:1, :]
    tail = jnp.exp(last) * product + jnp.sum(key_end * from_exit, axis=0, keepdims=True)
    ones = triangle(length, True).astype(jnp.float32)
    out_log[...] = dot(ones, query * grad_query - key * grad_key, 1, 0, highest) + tail
    out_query[...] = short(grad_query * query_scale)
    out_key[...] = short(grad_key)
    out_value[...] = short(grad_value)


def on_device(
    resid,
    norm_gain,
    cotangent,
    route_ids,
    route_weight,
    expert_gate,
    expert_up,
    expert_down,
    out_proj,
    mixed,
    query,
    key,
    value,
    log_decay,
    span_state,
):
    tokens_here = resid.shape[0]
    model_width = resid.shape[1]
    sp_count = lax.axis_size("sp")
    tp_count = lax.axis_size("tp")
    experts = sp_count * expert_gate.shape[0]
    capacity = 3 * tokens_here // experts
    resid_f = resid.astype(jnp.float32)
    inverse_rms = lax.rsqrt(jnp.mean(resid_f * resid_f, axis=1, keepdims=True) + epsilon)
    unit_rows = resid_f * inverse_rms
    normed = (unit_rows * norm_gain).astype(jnp.bfloat16)
    pair_expert = route_ids.reshape(-1)
    onehot = (pair_expert[:, None] == jnp.arange(experts, dtype=jnp.int32)[None, :]).astype(
        jnp.int32
    )
    slot_rank = jnp.sum((jnp.cumsum(onehot, axis=0) - onehot) * onehot, axis=1)
    slot_of = pair_expert * capacity + slot_rank
    slot_pairs = slot_of[None, :] == jnp.arange(experts * capacity, dtype=jnp.int32)[:, None]
    slot_tokens = jnp.any(slot_pairs.reshape(experts * capacity, tokens_here, TOP), axis=2).astype(
        jnp.bfloat16
    )
    slot_weight = jnp.sum(jnp.where(slot_pairs, route_weight.reshape(1, -1), 0.0), axis=1)
    column_share = model_width // tp_count
    offset = lax.axis_index("tp") * column_share
    rows_in = jnp.dot(
        slot_tokens,
        lax.dynamic_slice_in_dim(normed, offset, column_share, 1),
        preferred_element_type=jnp.float32,
    ).astype(jnp.bfloat16)
    rows_cot = (
        jnp.dot(
            slot_tokens,
            lax.dynamic_slice_in_dim(cotangent, offset, column_share, 1),
            preferred_element_type=jnp.float32,
        )
        * slot_weight[:, None]
    )
    arrived = tuple(
        lax.all_to_all(
            rows.reshape(experts, capacity, -1), "sp", split_axis=0, concat_axis=0, tiled=True
        ).reshape(1, experts * capacity, -1)
        for rows in (rows_in, rows_cot.astype(jnp.bfloat16))
    )
    mixed_all = lax.all_gather(mixed, "sp", axis=0, tiled=True)
    expert_in, expert_cot = (
        lax.all_gather(arrived[0], "tp", axis=2, tiled=True),
        lax.all_gather(arrived[1], "tp", axis=2, tiled=True),
    )
    gate_pre = jnp.einsum(
        "erd,edf->erf", expert_in, expert_gate, preferred_element_type=jnp.float32
    )
    up_pre = jnp.einsum("erd,edf->erf", expert_in, expert_up, preferred_element_type=jnp.float32)
    gate_sig = jax.nn.sigmoid(gate_pre)
    hidden = (gate_pre * gate_sig * up_pre).astype(jnp.bfloat16)
    grad_hidden = jnp.einsum(
        "erd,efd->erf", expert_cot, expert_down, preferred_element_type=jnp.float32
    )
    grad_up_act = (grad_hidden * gate_pre * gate_sig).astype(jnp.bfloat16)
    grad_gate_act = (grad_hidden * up_pre * gate_sig * (1.0 + gate_pre * (1.0 - gate_sig))).astype(
        jnp.bfloat16
    )
    grad_down_w = jnp.einsum("erf,erd->efd", hidden, expert_cot, preferred_element_type=jnp.float32)
    grad_gate_w = jnp.einsum(
        "erd,erf->edf", expert_in, grad_gate_act, preferred_element_type=jnp.float32
    )
    grad_up_w = jnp.einsum(
        "erd,erf->edf", expert_in, grad_up_act, preferred_element_type=jnp.float32
    )
    partial_value = jnp.einsum(
        "erf,edf->erd", grad_gate_act, expert_gate, preferred_element_type=jnp.float32
    )
    partial_value = partial_value + jnp.einsum(
        "erf,edf->erd", grad_up_act, expert_up, preferred_element_type=jnp.float32
    )
    partial_short = partial_value.astype(jnp.bfloat16)
    summed = (
        lax.psum_scatter(partial_short, "tp", scatter_dimension=2, tiled=True)
        .astype(jnp.float32)
        .astype(jnp.bfloat16)
    )
    returned = lax.all_to_all(
        summed.reshape(experts, capacity, -1), "sp", split_axis=0, concat_axis=0, tiled=True
    )
    flat_rows = returned.reshape(experts * capacity, -1)
    grad_normed = lax.all_gather(
        lax.dot_general(
            slot_tokens, flat_rows, (((0,), (0,)), ((), ())), preferred_element_type=jnp.float32
        ).astype(jnp.bfloat16),
        "tp",
        axis=1,
        tiled=True,
    ).astype(jnp.float32)
    scaled = grad_normed * norm_gain
    grad_resid = cotangent.astype(jnp.float32) + inverse_rms * (
        scaled - unit_rows * jnp.mean(scaled * unit_rows, axis=1, keepdims=True)
    )
    grad_resid = grad_resid.astype(jnp.bfloat16)
    resid_all = lax.all_to_all(grad_resid, "sp", split_axis=1, concat_axis=0, tiled=True)
    proj_all = lax.all_gather(out_proj, "sp", axis=0, tiled=True)
    heads = query.shape[1] // KEY_CHANNELS
    narrow = pl.BlockSpec((tokens_here, KEY_CHANNELS), lambda h: (0, h))
    wide = pl.BlockSpec((tokens_here, DV), lambda h: (0, h))
    rows_kept = KEY_CHANNELS + SIDE
    grad_mixed, cum, own = pl.pallas_call(
        summary_kernel,
        grid=(heads,),
        in_specs=[
            pl.BlockSpec((tokens_here, model_width), lambda h: (0, 0)),
            pl.BlockSpec((model_width, DV), lambda h: (0, h)),
            narrow,
            narrow,
        ],
        out_specs=[wide, narrow, pl.BlockSpec((1, rows_kept, DV), lambda h: (h, 0, 0))],
        out_shape=[
            jax.ShapeDtypeStruct((tokens_here, heads * DV), jnp.bfloat16),
            jax.ShapeDtypeStruct((tokens_here, heads * KEY_CHANNELS), jnp.float32),
            jax.ShapeDtypeStruct((heads, rows_kept, DV), jnp.bfloat16),
        ],
        cost_estimate=pl.CostEstimate(
            flops=2 * tokens_here * heads * DV * (model_width + 2 * KEY_CHANNELS),
            bytes_accessed=2 * model_width * heads * DV + 8 * tokens_here * heads * DV,
            transcendentals=tokens_here * heads * KEY_CHANNELS,
        ),
        name="summary",
    )(grad_resid, proj_all, query, log_decay)
    gathered = lax.all_gather(own, "sp")
    me = lax.axis_index("sp").reshape(1).astype(jnp.int32)
    grad_query, grad_key, grad_value, grad_log_decay = pl.pallas_call(
        gradient_kernel,
        grid=(heads,),
        in_specs=[
            pl.BlockSpec(memory_space=pltpu.SMEM),
            pl.BlockSpec((sp_count, 1, rows_kept, DV), lambda h: (0, h, 0, 0)),
            wide,
            narrow,
            narrow,
            wide,
            narrow,
            pl.BlockSpec((1, 1, KEY_CHANNELS, DV), lambda h: (0, h, 0, 0)),
        ],
        out_specs=[narrow, narrow, wide, narrow],
        out_shape=[
            jax.ShapeDtypeStruct(query.shape, jnp.bfloat16),
            jax.ShapeDtypeStruct(key.shape, jnp.bfloat16),
            jax.ShapeDtypeStruct(value.shape, jnp.bfloat16),
            jax.ShapeDtypeStruct(log_decay.shape, jnp.float32),
        ],
        cost_estimate=pl.CostEstimate(
            flops=40 * tokens_here * heads * DV * KEY_CHANNELS,
            bytes_accessed=2 * sp_count * heads * rows_kept * DV + 24 * tokens_here * heads * DV,
            transcendentals=5 * tokens_here * heads * KEY_CHANNELS,
        ),
        name="gradients",
    )(me, gathered, grad_mixed, query, key, value, cum, span_state)
    grad_out_proj = lax.dot_general(
        resid_all, mixed_all, (((0,), (0,)), ((), ())), preferred_element_type=jnp.float32
    )
    return (
        grad_gate_w.astype(jnp.bfloat16),
        grad_up_w.astype(jnp.bfloat16),
        grad_down_w.astype(jnp.bfloat16),
        grad_out_proj,
        grad_query,
        grad_key,
        grad_value,
        grad_log_decay,
    )


def solution(mesh):
    return jax.shard_map(
        on_device,
        mesh=mesh,
        in_specs=(
            P("sp", None),
            P(),
            P("sp", None),
            P("sp", None),
            P("sp", None),
            P("sp", None, "tp"),
            P("sp", None, "tp"),
            P("sp", "tp", None),
            P("sp", "tp"),
            P("sp", "tp"),
            P("sp", "tp"),
            P("sp", "tp"),
            P("sp", "tp"),
            P("sp", "tp"),
            P("sp", "tp", None, None),
        ),
        out_specs=(
            P("sp", None, "tp"),
            P("sp", None, "tp"),
            P("sp", "tp", None),
            P("sp", "tp"),
            P("sp", "tp"),
            P("sp", "tp"),
            P("sp", "tp"),
            P("sp", "tp"),
        ),
        check_vma=False,
    )
```

```python
import jax
import jax.numpy as jnp
from jax import lax
from jax.experimental import pallas as pl
from jax.sharding import PartitionSpec as P

KEY_CHANNELS = 128
DV = 256
TOP = 2


epsilon = 1e-06
highest = lax.Precision.HIGHEST


SIDE = 64


def triangle(length, upper):
    rows = lax.broadcasted_iota(jnp.int32, (length, length), 0)
    cols = lax.broadcasted_iota(jnp.int32, (length, length), 1)
    return rows <= cols if upper else rows >= cols


def dot(a, b, ca, cb, precision=None):
    return lax.dot_general(
        a, b, (((ca,), (cb,)), ((), ())), preferred_element_type=jnp.float32, precision=precision
    )


def short(values):
    return values.astype(jnp.bfloat16)


def summary_kernel(resid_ref, proj_ref, query_ref, decay_ref, grad_ref, cum_ref, out_ref):
    length = query_ref.shape[0]
    grad = short(dot(resid_ref[...], proj_ref[...], 1, 0))
    grad_ref[...] = grad
    ones = triangle(length, False).astype(jnp.float32)
    cum = dot(ones, decay_ref[...], 1, 0, highest)
    cum_ref[...] = cum
    query = query_ref[...].astype(jnp.float32) * KEY_CHANNELS ** (-0.5)
    out_ref[0, :, 0:DV] = short(dot(short(query * jnp.exp(cum)), grad, 0, 0))
    fill = jnp.ones((length, 2 * SIDE), jnp.float32)
    total = jnp.exp(dot(decay_ref[...], fill, 0, 0, highest))
    upper = short(total).astype(jnp.float32)
    lanes = lax.broadcasted_iota(jnp.int32, total.shape, 1)
    out_ref[0, :, DV : DV + 2 * SIDE] = short(jnp.where(lanes < SIDE, upper, total - upper))


def gradient_kernel(
    exit_ref, grad_ref, query_ref, key_ref, value_ref, cum_ref, state_ref,
    out_query, out_key, out_value, out_log,
):
    length = query_ref.shape[0]
    exit_short = exit_ref[0]
    exit_cot = exit_short.astype(jnp.float32)
    query_scale = KEY_CHANNELS ** (-0.5)
    cum = cum_ref[...]
    last = cum[length - 1 : length, :]
    middle = cum[length // 2 - 1 : length // 2, :]
    query = query_ref[...].astype(jnp.float32) * query_scale
    key = key_ref[...].astype(jnp.float32)
    grad = grad_ref[...]
    value = value_ref[...]
    state = state_ref[0, 0]
    rise = jnp.exp(cum - middle)
    fall = jnp.exp(middle - cum)
    to_end = jnp.exp(last - cum)
    causal = triangle(length, False)
    query_part = short(query * rise)
    key_part = short(key * fall)
    scores = short(jnp.where(causal, dot(query_part, key_part, 1, 1), 0.0))
    grad_scores = short(jnp.where(causal, dot(grad, value, 1, 1), 0.0))
    grad_query = rise * dot(grad_scores, key_part, 1, 0)
    grad_query = grad_query + jnp.exp(cum) * dot(grad, short(state), 1, 1)
    from_exit = dot(value, exit_short, 1, 1)
    key_end = key * to_end
    grad_key = fall * dot(grad_scores, query_part, 0, 0) + to_end * from_exit
    grad_value = dot(scores, grad, 0, 0) + dot(short(key_end), exit_short, 1, 0)
    product = dot(jnp.ones((8, DV), jnp.float32), state * exit_cot, 1, 1, highest)[0:1, :]
    tail = jnp.exp(last) * product + jnp.sum(key_end * from_exit, axis=0, keepdims=True)
    ones = triangle(length, True).astype(jnp.float32)
    out_log[...] = dot(ones, query * grad_query - key * grad_key, 1, 0, highest) + tail
    out_query[...] = short(grad_query * query_scale)
    out_key[...] = short(grad_key)
    out_value[...] = short(grad_value)


def on_device(
    resid,
    norm_gain,
    cotangent,
    route_ids,
    route_weight,
    expert_gate,
    expert_up,
    expert_down,
    out_proj,
    mixed,
    query,
    key,
    value,
    log_decay,
    span_state,
):
    tokens_here = resid.shape[0]
    model_width = resid.shape[1]
    sp_count = lax.axis_size("sp")
    tp_count = lax.axis_size("tp")
    experts = sp_count * expert_gate.shape[0]
    capacity = 3 * tokens_here // experts
    resid_f = resid.astype(jnp.float32)
    inverse_rms = lax.rsqrt(jnp.mean(resid_f * resid_f, axis=1, keepdims=True) + epsilon)
    unit_rows = resid_f * inverse_rms
    normed = (unit_rows * norm_gain).astype(jnp.bfloat16)
    pair_expert = route_ids.reshape(-1)
    onehot = (pair_expert[:, None] == jnp.arange(experts, dtype=jnp.int32)[None, :]).astype(
        jnp.int32
    )
    slot_rank = jnp.sum((jnp.cumsum(onehot, axis=0) - onehot) * onehot, axis=1)
    slot_of = pair_expert * capacity + slot_rank
    slot_pairs = slot_of[None, :] == jnp.arange(experts * capacity, dtype=jnp.int32)[:, None]
    slot_tokens = jnp.any(slot_pairs.reshape(experts * capacity, tokens_here, TOP), axis=2).astype(
        jnp.bfloat16
    )
    slot_weight = jnp.sum(jnp.where(slot_pairs, route_weight.reshape(1, -1), 0.0), axis=1)
    column_share = model_width // tp_count
    offset = lax.axis_index("tp") * column_share
    rows_in = jnp.dot(
        slot_tokens,
        lax.dynamic_slice_in_dim(normed, offset, column_share, 1),
        preferred_element_type=jnp.float32,
    ).astype(jnp.bfloat16)
    rows_cot = (
        jnp.dot(
            slot_tokens,
            lax.dynamic_slice_in_dim(cotangent, offset, column_share, 1),
            preferred_element_type=jnp.float32,
        )
        * slot_weight[:, None]
    )
    arrived = tuple(
        lax.all_to_all(
            rows.reshape(experts, capacity, -1), "sp", split_axis=0, concat_axis=0, tiled=True
        ).reshape(1, experts * capacity, -1)
        for rows in (rows_in, rows_cot.astype(jnp.bfloat16))
    )
    mixed_all = lax.all_gather(mixed, "sp", axis=0, tiled=True)
    expert_in, expert_cot = (
        lax.all_gather(arrived[0], "tp", axis=2, tiled=True),
        lax.all_gather(arrived[1], "tp", axis=2, tiled=True),
    )
    gate_pre = jnp.einsum(
        "erd,edf->erf", expert_in, expert_gate, preferred_element_type=jnp.float32
    )
    up_pre = jnp.einsum("erd,edf->erf", expert_in, expert_up, preferred_element_type=jnp.float32)
    gate_sig = jax.nn.sigmoid(gate_pre)
    hidden = (gate_pre * gate_sig * up_pre).astype(jnp.bfloat16)
    grad_hidden = jnp.einsum(
        "erd,efd->erf", expert_cot, expert_down, preferred_element_type=jnp.float32
    )
    grad_up_act = (grad_hidden * gate_pre * gate_sig).astype(jnp.bfloat16)
    grad_gate_act = (grad_hidden * up_pre * gate_sig * (1.0 + gate_pre * (1.0 - gate_sig))).astype(
        jnp.bfloat16
    )
    grad_down_w = jnp.einsum("erf,erd->efd", hidden, expert_cot, preferred_element_type=jnp.float32)
    grad_gate_w = jnp.einsum(
        "erd,erf->edf", expert_in, grad_gate_act, preferred_element_type=jnp.float32
    )
    grad_up_w = jnp.einsum(
        "erd,erf->edf", expert_in, grad_up_act, preferred_element_type=jnp.float32
    )
    partial_value = jnp.einsum(
        "erf,edf->erd", grad_gate_act, expert_gate, preferred_element_type=jnp.float32
    )
    partial_value = partial_value + jnp.einsum(
        "erf,edf->erd", grad_up_act, expert_up, preferred_element_type=jnp.float32
    )
    partial_short = partial_value.astype(jnp.bfloat16)
    summed = (
        lax.psum_scatter(partial_short, "tp", scatter_dimension=2, tiled=True)
        .astype(jnp.float32)
        .astype(jnp.bfloat16)
    )
    returned = lax.all_to_all(
        summed.reshape(experts, capacity, -1), "sp", split_axis=0, concat_axis=0, tiled=True
    )
    flat_rows = returned.reshape(experts * capacity, -1)
    grad_normed = lax.all_gather(
        lax.dot_general(
            slot_tokens, flat_rows, (((0,), (0,)), ((), ())), preferred_element_type=jnp.float32
        ).astype(jnp.bfloat16),
        "tp",
        axis=1,
        tiled=True,
    ).astype(jnp.float32)
    scaled = grad_normed * norm_gain
    grad_resid = cotangent.astype(jnp.float32) + inverse_rms * (
        scaled - unit_rows * jnp.mean(scaled * unit_rows, axis=1, keepdims=True)
    )
    grad_resid = grad_resid.astype(jnp.bfloat16)
    resid_all = lax.all_to_all(grad_resid, "sp", split_axis=1, concat_axis=0, tiled=True)
    proj_all = lax.all_gather(out_proj, "sp", axis=0, tiled=True)
    heads = query.shape[1] // KEY_CHANNELS
    narrow = pl.BlockSpec((tokens_here, KEY_CHANNELS), lambda h: (0, h))
    wide = pl.BlockSpec((tokens_here, DV), lambda h: (0, h))
    packed = DV + 2 * SIDE
    grad_mixed, cum, own = pl.pallas_call(
        summary_kernel,
        grid=(heads,),
        in_specs=[
            pl.BlockSpec((tokens_here, model_width), lambda h: (0, 0)),
            pl.BlockSpec((model_width, DV), lambda h: (0, h)),
            narrow,
            narrow,
        ],
        out_specs=[wide, narrow, pl.BlockSpec((1, KEY_CHANNELS, packed), lambda h: (h, 0, 0))],
        out_shape=[
            jax.ShapeDtypeStruct((tokens_here, heads * DV), jnp.bfloat16),
            jax.ShapeDtypeStruct((tokens_here, heads * KEY_CHANNELS), jnp.float32),
            jax.ShapeDtypeStruct((heads, KEY_CHANNELS, packed), jnp.bfloat16),
        ],
        cost_estimate=pl.CostEstimate(
            flops=2 * tokens_here * heads * DV * (model_width + 2 * KEY_CHANNELS),
            bytes_accessed=2 * model_width * heads * DV + 8 * tokens_here * heads * DV,
            transcendentals=tokens_here * heads * KEY_CHANNELS,
        ),
        name="summary",
    )(grad_resid, proj_all, query, log_decay)
    share = KEY_CHANNELS // sp_count
    own_rows = own.reshape(heads, sp_count, share, packed).transpose(1, 0, 2, 3)
    spans = lax.all_to_all(
        own_rows.reshape(sp_count, heads * share, packed),
        "sp",
        split_axis=0,
        concat_axis=0,
        tiled=True,
    ).astype(jnp.float32)
    running = jnp.zeros((heads * share, DV), jnp.float32)
    exits = [running]
    for span in range(sp_count - 1, 0, -1):
        factor = spans[span, :, DV : DV + 1] + spans[span, :, DV + SIDE : DV + SIDE + 1]
        running = spans[span, :, :DV] + factor * running
        exits.append(running)
    exit_rows = lax.all_to_all(
        jnp.stack(exits[::-1]).astype(jnp.bfloat16),
        "sp",
        split_axis=0,
        concat_axis=0,
        tiled=True,
    )
    exit_all = (
        exit_rows.reshape(sp_count, heads, share, DV)
        .transpose(1, 0, 2, 3)
        .reshape(heads, KEY_CHANNELS, DV)
    )
    grad_query, grad_key, grad_value, grad_log_decay = pl.pallas_call(
        gradient_kernel,
        grid=(heads,),
        in_specs=[
            pl.BlockSpec((1, KEY_CHANNELS, DV), lambda h: (h, 0, 0)),
            wide,
            narrow,
            narrow,
            wide,
            narrow,
            pl.BlockSpec((1, 1, KEY_CHANNELS, DV), lambda h: (0, h, 0, 0)),
        ],
        out_specs=[narrow, narrow, wide, narrow],
        out_shape=[
            jax.ShapeDtypeStruct(query.shape, jnp.bfloat16),
            jax.ShapeDtypeStruct(key.shape, jnp.bfloat16),
            jax.ShapeDtypeStruct(value.shape, jnp.bfloat16),
            jax.ShapeDtypeStruct(log_decay.shape, jnp.float32),
        ],
        cost_estimate=pl.CostEstimate(
            flops=40 * tokens_here * heads * DV * KEY_CHANNELS,
            bytes_accessed=2 * heads * KEY_CHANNELS * DV + 24 * tokens_here * heads * DV,
            transcendentals=5 * tokens_here * heads * KEY_CHANNELS,
        ),
        name="gradients",
    )(exit_all, grad_mixed, query, key, value, cum, span_state)
    grad_out_proj = lax.dot_general(
        resid_all, mixed_all, (((0,), (0,)), ((), ())), preferred_element_type=jnp.float32
    )
    return (
        grad_gate_w.astype(jnp.bfloat16),
        grad_up_w.astype(jnp.bfloat16),
        grad_down_w.astype(jnp.bfloat16),
        grad_out_proj,
        grad_query,
        grad_key,
        grad_value,
        grad_log_decay,
    )


def solution(mesh):
    return jax.shard_map(
        on_device,
        mesh=mesh,
        in_specs=(
            P("sp", None),
            P(),
            P("sp", None),
            P("sp", None),
            P("sp", None),
            P("sp", None, "tp"),
            P("sp", None, "tp"),
            P("sp", "tp", None),
            P("sp", "tp"),
            P("sp", "tp"),
            P("sp", "tp"),
            P("sp", "tp"),
            P("sp", "tp"),
            P("sp", "tp"),
            P("sp", "tp", None, None),
        ),
        out_specs=(
            P("sp", None, "tp"),
            P("sp", None, "tp"),
            P("sp", "tp", None),
            P("sp", "tp"),
            P("sp", "tp"),
            P("sp", "tp"),
            P("sp", "tp"),
            P("sp", "tp"),
        ),
        check_vma=False,
    )
```
